32 devices in a mesh: grp: 2 (over x), sp: 4 (over z), tp: 4 (over y, core).
Axes of the slice: x: 2, y: 2, z: 4, core: 2. Of those that a mesh axis runs over, the one named last changes fastest.
Arguments:
- prompt_layer_input: bfloat16 [24, 512, 2048], P('grp', 'sp'), parts along dimension 0, may hold values from -10 to 10
- next_token_input: bfloat16 [24, 2048], P('grp'), parts along dimension 0, may hold values from -6 to 6
- value_projection: bfloat16 [2048, 2048], P(None, 'tp'), may hold values from -0.125 to 0.125
- output_gate_matrix: bfloat16 [2048, 2048], P(None, 'tp'), may hold values from -0.125 to 0.125
- key_projection: bfloat16 [2048, 256], replicated, may hold values from -0.0390625 to 0.0390625
- query_projection: bfloat16 [2048, 256], replicated, may hold values from -0.125 to 0.125
- step_projection: bfloat16 [2048, 32], replicated, may hold values from -0.125 to 0.125
- value_filter_taps: bfloat16 [4, 2048], replicated, may hold values from -3 to 3
- key_filter_taps: bfloat16 [4, 256], replicated, may hold values from -3 to 3
- query_filter_taps: bfloat16 [4, 256], replicated, may hold values from -3 to 3
- step_size_bias: float32 [32], replicated, may hold values from -4.3 to -0.7
- head_decay_logarithm: float32 [32], replicated, may hold values from -8.5 to -0.5
- direct_path_weight: float32 [32], replicated, may hold values from 0.1 to 1.9
- gated_norm_gain: float32 [32, 64], replicated, may hold values from 0.1 to 1.9
- position_decay_offset: float32 [24, 512, 32], P('grp', 'sp'), parts along dimension 0, may hold values from -2.1 to 0
Outputs:
- state_cache: bfloat16 [24, 32, 64, 128], P('grp', 'tp', 'sp'), parts along dimension 0
- first_read: bfloat16 [24, 32, 64], P('grp', 'tp', 'sp'), parts along dimension 0
The draws below stay inside these ranges and needn't reach their ends.
There are 2 independent parts, one for each index of `grp`. The reference program is written for one: setup_inputs(seed, part) draws one part's arguments, and reference() takes and returns one part's arrays. A program takes and returns all parts, laid end to end along the dimension named above; an argument that names none is the same for every part. Nothing has to cross between parts.
All inputs are finite; a program needn't handle non-finite values.
Results may differ from the reference program's by a relative error of at most 0.011.
Values may be sent and summed in bfloat16 or wider, within the bound.
A program may use at most 64 MiB of HBM per device.

```python
import math
import jax
import jax.numpy as jnp
from jax import lax

D = 2048
HEADS = 32
P_SIZE = 64
GROUPS = 2
STATE = 128
CONV = 4
SPAN = 64
SEQS = 12
LEN = 512


def head_speeds(key, fast_share):
    return jax.random.uniform(jax.random.fold_in(key, 11), (HEADS,), jnp.float32) < fast_share


def draw_step_size_bias(key, part):
    fast_share = 0.5
    fast_heads = head_speeds(key, fast_share)
    jitter = jax.random.uniform(jax.random.fold_in(key, 12), (HEADS,), jnp.float32, -0.3, 0.3)
    return (jnp.where(fast_heads, -1.0, -4.0) + jitter).astype(jnp.float32)


def draw_head_decay_logarithm(key, part):
    fast_share = 0.5
    fast_heads = head_speeds(key, fast_share)
    fraction = jax.random.uniform(jax.random.fold_in(key, 13), (HEADS,), jnp.float32)
    fast_rate = jnp.exp(math.log(0.01) + fraction * math.log(10.0 / 3.0)) / 0.4
    slow_rate = jnp.exp(math.log(0.1 / LEN) + fraction * math.log(6.0)) / 0.035
    return jnp.log(jnp.where(fast_heads, fast_rate, slow_rate)).astype(jnp.float32)


def draw_prompt_layer_input(key, part):
    block_count = LEN // SPAN
    drawn_draw = jnp.clip(jax.random.normal(jax.random.fold_in(key, 21), (SEQS, LEN, D), jnp.float32), -6.0, 6.0)
    spread = jnp.exp(jax.random.uniform(jax.random.fold_in(key, 22), (SEQS, block_count), jnp.float32, math.log(0.6), math.log(1.6)))
    shaped = drawn_draw.reshape(SEQS, block_count, SPAN, D) * spread[:, :, None, None]
    return shaped.reshape(SEQS, LEN, D).astype(jnp.bfloat16)


def draw_position_decay_offset(key, part):
    positions = jax.random.randint(jax.random.fold_in(key, 31), (SEQS, 3, HEADS), 0, LEN)
    strength = jax.random.uniform(jax.random.fold_in(key, 32), (SEQS, 3, HEADS), jnp.float32, math.log(0.5), math.log(0.8))
    places = jnp.arange(LEN, dtype=jnp.int32)
    matched = places[None, :, None, None] == positions[:, None, :, :]
    return jnp.sum(jnp.where(matched, strength[:, None], 0.0), axis=2).astype(jnp.float32)


def steps_of(own_key, dims, cuts, least, top_value):
    loudness = 1.0
    for axis_at, shards_of in cuts:
        heights = jax.random.uniform(jax.random.fold_in(jax.random.fold_in(own_key, 6), axis_at), (shards_of,), jnp.float32, least / len(cuts), top_value / len(cuts))
        loudness = loudness * jnp.repeat(jnp.exp(heights), dims[axis_at] // shards_of).reshape((-1,) + (1,) * (len(dims) - 1 - axis_at))
    return loudness


def gaussian(key, shape, scale, limit, cuts=(), kind=jnp.bfloat16):
    values = scale * jax.random.normal(key, shape, jnp.float32)
    if cuts:
        values = values * steps_of(key, shape, cuts, -0.22, 0.18)
    return jnp.clip(values, -limit, limit).astype(kind)


def setup_inputs(seed: int = 0, part: int = 0) -> dict:
    splits = jax.random.split(jax.random.key(seed), 16)
    part_keys = jax.random.split(jax.random.fold_in(splits[15], part), 16)
    return {
        "prompt_layer_input": draw_prompt_layer_input(jax.random.fold_in(jax.random.fold_in(splits[15], part), 71), part),
        "next_token_input": gaussian(part_keys[1], (SEQS, D), 1.0, 6.0),
        "value_projection": gaussian(splits[2], (D, HEADS * P_SIZE), D ** -0.5, 0.125, ((1, 4),)),
        "output_gate_matrix": gaussian(splits[3], (D, HEADS * P_SIZE), D ** -0.5, 0.125, ((1, 4),)),
        "key_projection": gaussian(splits[4], (D, GROUPS * STATE), (11 * D) ** -0.5, 0.0390625),
        "query_projection": gaussian(splits[5], (D, GROUPS * STATE), D ** -0.5, 0.125),
        "step_projection": gaussian(splits[6], (D, HEADS), D ** -0.5, 0.125),
        "value_filter_taps": gaussian(splits[7], (CONV, HEADS * P_SIZE), 0.5, 3.0),
        "key_filter_taps": gaussian(splits[8], (CONV, GROUPS * STATE), 0.5, 3.0),
        "query_filter_taps": gaussian(splits[9], (CONV, GROUPS * STATE), 0.5, 3.0),
        "step_size_bias": draw_step_size_bias(jax.random.fold_in(splits[15], 71), part),
        "head_decay_logarithm": draw_head_decay_logarithm(jax.random.fold_in(splits[15], 71), part),
        "direct_path_weight": jnp.clip(1.0 + 0.18 * jax.random.normal(splits[12], (HEADS,), jnp.float32), 0.1, 1.9),
        "gated_norm_gain": jnp.clip(1.0 + 0.18 * jax.random.normal(splits[13], (HEADS, P_SIZE), jnp.float32), 0.1, 1.9),
        "position_decay_offset": draw_position_decay_offset(jax.random.fold_in(jax.random.fold_in(splits[15], part), 71), part),
    }


epsilon = 1e-06

def reference(prompt_layer_input, next_token_input, value_projection, output_gate_matrix, key_projection, query_projection, step_projection, value_filter_taps, key_filter_taps, query_filter_taps, step_size_bias, head_decay_logarithm, direct_path_weight, gated_norm_gain, position_decay_offset):
    seq_count, length, width = prompt_layer_input.shape
    feature_cols = HEADS * P_SIZE
    map_cols = GROUPS * STATE
    weights_all = jnp.concatenate([value_projection, key_projection, query_projection], axis=1)
    kernel = jnp.concatenate([value_filter_taps, key_filter_taps, query_filter_taps], axis=1).astype(jnp.float32)
    token_rows = prompt_layer_input.reshape(seq_count * length, width)
    projected = jnp.dot(token_rows, weights_all, preferred_element_type=jnp.float32).astype(jnp.bfloat16)
    projected = projected.reshape(seq_count, length, feature_cols + 2 * map_cols)
    step_raw = jnp.dot(token_rows, step_projection, preferred_element_type=jnp.float32).astype(jnp.bfloat16)
    step_raw = step_raw.reshape(seq_count, length, HEADS)
    padded = jnp.concatenate([jnp.zeros((seq_count, CONV - 1, feature_cols + 2 * map_cols), jnp.bfloat16), projected], axis=1)
    total = padded[:, 0:length].astype(jnp.float32) * kernel[0]
    for tap in range(1, CONV):
        total = total + padded[:, tap:tap + length].astype(jnp.float32) * kernel[tap]
    mixed = jax.nn.silu(total).astype(jnp.bfloat16)
    head_decay_speed = jnp.exp(head_decay_logarithm)
    discrete_step = jax.nn.softplus(step_raw.astype(jnp.float32) + step_size_bias)
    logarithmic_decay = position_decay_offset - head_decay_speed * discrete_step
    head_input = mixed[:, :, :feature_cols].reshape(seq_count, length, HEADS, P_SIZE)
    in_map = mixed[:, :, feature_cols:feature_cols + map_cols].reshape(seq_count, length, GROUPS, STATE)
    block_count = length // SPAN

    def blocks(array):
        return jnp.moveaxis(array.reshape((seq_count, block_count, SPAN) + array.shape[2:]), 1, 0)

    def advance(carry, inputs):
        input_block, map_block, step_block, decay_block = inputs
        cumulative = jnp.cumsum(decay_block, axis=1)
        decay_weight = jnp.exp(cumulative[:, -1:] - cumulative) * step_block
        weighted = (input_block.astype(jnp.float32) * decay_weight[..., None]).astype(jnp.bfloat16)
        head_map = jnp.repeat(map_block, HEADS // GROUPS, axis=2)
        block_state = jnp.einsum('bshp,bshn->bhpn', weighted.astype(jnp.float32), head_map.astype(jnp.float32))
        return (jnp.exp(cumulative[:, -1])[:, :, None, None] * carry + block_state, None)
    final, unused = lax.scan(advance, jnp.zeros((seq_count, HEADS, P_SIZE, STATE), jnp.float32), (blocks(head_input), blocks(in_map), blocks(discrete_step), blocks(logarithmic_decay)))
    state_cache = final.astype(jnp.bfloat16)
    new_raw = jnp.dot(next_token_input, weights_all, preferred_element_type=jnp.float32).astype(jnp.bfloat16)
    new_step = jnp.dot(next_token_input, step_projection, preferred_element_type=jnp.float32).astype(jnp.bfloat16)
    new_gate = jnp.dot(next_token_input, output_gate_matrix, preferred_element_type=jnp.float32).astype(jnp.bfloat16)
    window = jnp.concatenate([projected[:, length - (CONV - 1):], new_raw[:, None]], axis=1)
    new_mixed = jax.nn.silu(lax.optimization_barrier(jnp.sum(window.astype(jnp.float32) * kernel[None], axis=1))).astype(jnp.bfloat16)
    new_input = new_mixed[:, :feature_cols].reshape(seq_count, HEADS, P_SIZE).astype(jnp.float32)
    new_in = jnp.repeat(new_mixed[:, feature_cols:feature_cols + map_cols].reshape(seq_count, GROUPS, STATE), HEADS // GROUPS, axis=1).astype(jnp.float32)
    new_out = jnp.repeat(new_mixed[:, feature_cols + map_cols:].reshape(seq_count, GROUPS, STATE), HEADS // GROUPS, axis=1).astype(jnp.float32)
    new_step_size = jax.nn.softplus(new_step.astype(jnp.float32) + step_size_bias)
    cache_values = lax.optimization_barrier(state_cache).astype(jnp.float32)
    new_state = jnp.exp(-head_decay_speed * new_step_size)[:, :, None, None] * cache_values + (new_step_size[:, :, None] * new_input)[..., None] * new_in[:, :, None, :]
    readout = lax.optimization_barrier(jnp.sum(new_state * new_out[:, :, None, :], axis=-1)) + direct_path_weight[None, :, None] * new_input
    gated = readout * jax.nn.silu(new_gate.astype(jnp.float32).reshape(seq_count, HEADS, P_SIZE))
    scale = lax.rsqrt(lax.optimization_barrier(jnp.mean(gated * gated, axis=(1, 2), keepdims=True)) + epsilon)
    first_read = (gated * scale * gated_norm_gain[None]).astype(jnp.bfloat16)
    return (state_cache, first_read)
```

```python
import jax
import jax.numpy as jnp
from jax import lax
from jax.experimental import pallas as pl
from jax.experimental.pallas import tpu as pltpu
from jax.sharding import PartitionSpec as P

HEADS = 32
P_SIZE = 64
GROUPS = 2
STATE = 128
CONV = 4
SPAN = 64


epsilon = 1e-06


def shifted(block, axis, distance):
    devices = range(lax.axis_size(axis))
    route = [(i - distance, i) for i in devices if i - distance in devices]
    return lax.ppermute(block, axis, route)


def broadcast(value, axis, source):
    kept = jnp.where(lax.axis_index(axis) == source, value, 0).astype(value.dtype)
    return lax.psum(kept, axis)


def prefix(shard, axis, combine, identity):
    length, here = (lax.axis_size(axis), lax.axis_index(axis))
    everything = lax.all_gather(shard, axis)
    start = jnp.broadcast_to(jnp.asarray(identity, shard.dtype), shard.shape)

    def lap(k, before):
        at = length - 1 - k
        reached = at > here
        new = combine(before, everything[at])
        return jnp.where(reached, new, before)

    return lax.fori_loop(0, length, lap, start)


def shards(
    prompt_layer_input,
    next_token_input,
    value_projection,
    output_gate_matrix,
    key_projection,
    query_projection,
    step_projection,
    value_filter_taps,
    key_filter_taps,
    query_filter_taps,
    step_size_bias,
    head_decay_logarithm,
    direct_path_weight,
    gated_norm_gain,
    position_decay_offset,
):
    seq_count, local_len, width = prompt_layer_input.shape
    resident_heads = value_projection.shape[1] // P_SIZE
    feature_cols = resident_heads * P_SIZE
    shard_count = lax.axis_size("sp")
    rows_here = P_SIZE // shard_count
    shard_index = lax.axis_index("sp")
    leading_head = lax.axis_index("tp") * resident_heads
    group_index = leading_head // (HEADS // GROUPS)
    row_first = shard_index * rows_here
    in_cols = lax.dynamic_slice_in_dim(key_projection, group_index * STATE, STATE, 1)
    out_cols = lax.dynamic_slice_in_dim(query_projection, group_index * STATE, STATE, 1)
    weights_here = jnp.concatenate([value_projection, in_cols, out_cols], axis=1)
    step_cols = lax.dynamic_slice_in_dim(step_projection, leading_head, resident_heads, 1)
    kernel = jnp.concatenate(
        [
            lax.dynamic_slice_in_dim(value_filter_taps, leading_head * P_SIZE, feature_cols, 1),
            lax.dynamic_slice_in_dim(key_filter_taps, group_index * STATE, STATE, 1),
            lax.dynamic_slice_in_dim(query_filter_taps, group_index * STATE, STATE, 1),
        ],
        axis=1,
    ).astype(jnp.float32)
    head_decay_speed = jnp.exp(
        lax.dynamic_slice_in_dim(head_decay_logarithm, leading_head, resident_heads, 0)
    )
    bias_here = lax.dynamic_slice_in_dim(step_size_bias, leading_head, resident_heads, 0)
    skip_here = lax.dynamic_slice_in_dim(direct_path_weight, leading_head, resident_heads, 0)
    gain_here = lax.dynamic_slice(
        gated_norm_gain, (leading_head, row_first), (resident_heads, rows_here)
    )
    token_rows = prompt_layer_input.reshape(seq_count * local_len, width)
    projected = jnp.dot(token_rows, weights_here, preferred_element_type=jnp.float32).astype(
        jnp.bfloat16
    )
    projected = projected.reshape(seq_count, local_len, feature_cols + 2 * STATE)
    trailing = projected[:, local_len - (CONV - 1) :]
    before = shifted(trailing, "sp", 1)
    newest = broadcast(trailing, "sp", shard_count - 1)
    padded = jnp.concatenate([before, projected], axis=1)
    total = padded[:, 0:local_len].astype(jnp.float32) * kernel[0]
    for tap in range(1, CONV):
        total = total + padded[:, tap : tap + local_len].astype(jnp.float32) * kernel[tap]
    mixed = jax.nn.silu(total).astype(jnp.bfloat16)
    step_raw = jnp.dot(token_rows, step_cols, preferred_element_type=jnp.float32).astype(
        jnp.bfloat16
    )
    discrete_step = jax.nn.softplus(step_raw.astype(jnp.float32) + bias_here).reshape(
        seq_count, local_len, resident_heads
    )
    decay_spikes = lax.dynamic_slice_in_dim(position_decay_offset, leading_head, resident_heads, 2)
    logarithmic_decay = decay_spikes - head_decay_speed * discrete_step
    block_count = local_len // SPAN
    cumulative = jnp.cumsum(
        logarithmic_decay.reshape(seq_count, block_count, SPAN, resident_heads), axis=2
    )
    decay_weight = jnp.exp(cumulative[:, :, -1:] - cumulative) * discrete_step.reshape(
        seq_count, block_count, SPAN, resident_heads
    )
    head_input = mixed[:, :, :feature_cols].reshape(
        seq_count, block_count, SPAN, resident_heads, P_SIZE
    )
    weighted = (head_input.astype(jnp.float32) * decay_weight[..., None]).astype(jnp.bfloat16)
    in_map = mixed[:, :, feature_cols : feature_cols + STATE].reshape(
        seq_count, block_count, SPAN, STATE
    )
    block_state = jnp.einsum(
        "bcshp,bcsn->bchpn", weighted, in_map, preferred_element_type=jnp.float32
    )
    block_log = cumulative[:, :, -1]
    own_log = jnp.sum(block_log, axis=1)
    after_block = jnp.exp(own_log[:, None] - jnp.cumsum(block_log, axis=1))
    local_state = jnp.sum(after_block[..., None, None] * block_state, axis=1)
    later_log = prefix(own_log, "sp", jnp.add, jnp.zeros_like(own_log))
    scaled = jnp.exp(later_log)[:, :, None, None] * local_state
    own_rows = lax.psum_scatter(scaled, "sp", scatter_dimension=2, tiled=True)
    state_cache = own_rows.astype(jnp.bfloat16)
    new_raw = jnp.dot(next_token_input, weights_here, preferred_element_type=jnp.float32).astype(
        jnp.bfloat16
    )
    new_step = jnp.dot(next_token_input, step_cols, preferred_element_type=jnp.float32).astype(
        jnp.bfloat16
    )
    new_gate = jnp.dot(
        next_token_input, output_gate_matrix, preferred_element_type=jnp.float32
    ).astype(jnp.bfloat16)
    window = jnp.concatenate([newest, new_raw[:, None]], axis=1)
    new_mixed = jax.nn.silu(jnp.sum(window.astype(jnp.float32) * kernel[None], axis=1)).astype(
        jnp.bfloat16
    )
    new_input = lax.dynamic_slice_in_dim(
        new_mixed[:, :feature_cols].reshape(seq_count, resident_heads, P_SIZE),
        row_first,
        rows_here,
        2,
    ).astype(jnp.float32)
    new_in = new_mixed[:, feature_cols : feature_cols + STATE].astype(jnp.float32)
    new_out = new_mixed[:, feature_cols + STATE :].astype(jnp.float32)
    new_step_size = jax.nn.softplus(new_step.astype(jnp.float32) + bias_here)
    cache_values = lax.optimization_barrier(state_cache).astype(jnp.float32)
    new_state = (
        jnp.exp(-head_decay_speed * new_step_size)[:, :, None, None] * cache_values
        + (new_step_size[:, :, None] * new_input)[..., None] * new_in[:, None, None, :]
    )
    readout = (
        jnp.sum(new_state * new_out[:, None, None, :], axis=-1)
        + skip_here[None, :, None] * new_input
    )
    gate_rows = lax.dynamic_slice_in_dim(
        new_gate.reshape(seq_count, resident_heads, P_SIZE), row_first, rows_here, 2
    )
    gated = readout * jax.nn.silu(gate_rows.astype(jnp.float32))
    squares = lax.psum(jnp.sum(gated * gated, axis=(1, 2)), ("sp", "tp"))
    scale = lax.rsqrt(squares / (HEADS * P_SIZE) + epsilon)
    first_read = (gated * scale[:, None, None] * gain_here[None]).astype(jnp.bfloat16)
    return (state_cache, first_read)


F32, BF16 = jnp.float32, jnp.bfloat16
MESH = pl.DeviceIdType.MESH
EXACT = lax.Precision.HIGHEST


def exact_dot(a, b, dims=((1,), (0,))):
    return lax.dot_general(a, b, (dims, ((), ())), precision=EXACT, preferred_element_type=F32)


def softplus(v):
    return jnp.maximum(v, 0.0) + jnp.log1p(jnp.exp(-jnp.abs(v)))


def silu(v):
    return v / (1.0 + jnp.exp(-v))


def ones_where(shape, test, dtype=F32):
    rows = lax.broadcasted_iota(jnp.int32, shape, 0)
    cols = lax.broadcasted_iota(jnp.int32, shape, 1)
    return jnp.where(test(rows, cols), 1.0, 0.0).astype(dtype)


def mixer_kernel(
    dims,
    x_hbm,
    next_ref,
    wv_hbm,
    wg_hbm,
    wk_hbm,
    wq_hbm,
    ws_hbm,
    tv_ref,
    tk_ref,
    tq_ref,
    bias_ref,
    speed_ref,
    skip_ref,
    gain_ref,
    off_hbm,
    cache_ref,
    read_ref,
    xbuf,
    edge,
    wall,
    wq,
    ws,
    wg,
    off,
    taps,
    pad,
    halo_out,
    halo_in,
    halo,
    newest,
    logs_out,
    logs,
    sendbuf,
    recv,
    sq_out,
    sq_in,
    expand,
    load_sem,
    x_sem,
    halo_sem,
    new_send,
    new_recv,
    st_send,
    st_recv,
    log_send,
    log_recv,
    sq_send,
    sq_recv,
):
    n, m, S, L, heads, R, G = dims
    F = heads * P_SIZE
    C = F + STATE
    SP = sq_out.shape[0]
    steps = S // G
    me, tp = lax.axis_index("sp"), lax.axis_index("tp")
    lead = tp * heads
    group = lax.div(lead, HEADS // GROUPS)
    fcol = pl.multiple_of(tp * F, 128)
    gcol = pl.multiple_of(group * STATE, 128)

    def load(src, dst, k):
        c = pltpu.make_async_copy(src, dst, load_sem.at[k])
        c.start()
        return c

    def load_x(g):
        return pltpu.make_async_copy(
            x_hbm.at[pl.ds(g * G, G)], xbuf.at[pl.ds(g * G, G)], x_sem.at[g]
        )

    first = [
        load(x_hbm.at[:, pl.ds(L - 16, 16)], edge.at[pl.ds(0, S)], 0),
        load(wk_hbm.at[:, pl.ds(gcol, STATE)], wall.at[:, pl.ds(F, STATE)], 1),
        load(ws_hbm, ws, 2),
        load(wq_hbm.at[:, pl.ds(gcol, STATE)], wq, 3),
        load(wv_hbm, wall.at[:, pl.ds(0, F)], 4),
    ]
    for g in range(steps):
        load_x(g).start()
    off_load = load(off_hbm, off, 5)
    gate_load = load(wg_hbm, wg, 6)

    peers = [(a, b) for a in range(n) for b in range(m) if (a, b) != (0, 0)]

    def at(a, b=0):
        return {"sp": lax.rem(me + a, n), "tp": lax.rem(tp + b, m)}

    barrier = pltpu.get_barrier_semaphore()
    for a, b in peers:
        pl.semaphore_signal(barrier, inc=1, device_id=at(a, b), device_id_type=MESH)

    taps[:, 0:F] = tv_ref[:, pl.ds(fcol, F)].astype(F32)
    taps[:, F:C] = tk_ref[:, pl.ds(gcol, STATE)].astype(F32)
    taps[:, C : C + STATE] = tq_ref[:, pl.ds(gcol, STATE)].astype(F32)
    edge[S] = jnp.zeros(edge.shape[1:], BF16)
    edge[S, 0:S, :] = next_ref[...]
    logs_out[...] = jnp.zeros_like(logs_out)
    halo_out[...] = jnp.zeros_like(halo_out)
    newest_zero = jnp.zeros(newest.shape[1:], F32)
    head_of = ones_where((HEADS, F), lambda i, c: i == lead + lax.div(c, P_SIZE), BF16)
    expand[0:HEADS, :] = head_of
    expand[HEADS : 2 * HEADS, :] = head_of
    bias = bias_ref[...]
    speed = jnp.exp(speed_ref[...])

    for c in first:
        c.wait()
    wall[:, C : C + STATE] = jnp.concatenate(
        [ws[...], jnp.zeros((ws.shape[0], STATE - HEADS), BF16)], axis=1
    )
    rows = edge[...].reshape((S + 1) * 16, edge.shape[2])
    eproj = jnp.dot(rows, wall[...], preferred_element_type=F32).astype(BF16).astype(F32)
    eq = jnp.dot(rows, wq[...], preferred_element_type=F32).astype(BF16).astype(F32)
    e3 = eproj.reshape(S + 1, 16, C + STATE)
    q3 = eq.reshape(S + 1, 16, STATE)
    total = jnp.zeros((S, C + STATE), F32)
    for j in range(CONV - 1):
        row = 16 - (CONV - 1) + j
        tail = e3[0:S, row, 0:C]
        halo_out[j, 0:S, :] = tail.astype(BF16)
        total = total + jnp.concatenate([tail, q3[0:S, row, :]], axis=1) * taps[j : j + 1, :]
    new_raw = jnp.concatenate([e3[S, :, 0:C], q3[S]], axis=1)
    new_step = e3[S, :, C : C + HEADS]

    pl.semaphore_wait(barrier, len(peers))

    def halo_copy():
        return pltpu.make_async_remote_copy(
            halo_out, halo_in, halo_sem.at[0], halo_sem.at[1], device_id=at(1), device_id_type=MESH
        )

    @pl.when(me < n - 1)
    def _():
        halo_copy().start()

    def newest_copy(k):
        return pltpu.make_async_remote_copy(
            newest, newest, new_send.at[k], new_recv, device_id=at(k), device_id_type=MESH
        )

    @pl.when(me == n - 1)
    def _():
        newest[0] = newest_zero
        newest[0, 0:S, :] = total
        for k in range(1, n):
            newest_copy(k).start()

    def state_copy(g, k):
        to = lax.rem(me + k, n)
        return pltpu.make_async_remote_copy(
            sendbuf.at[to, pl.ds(g * G, G)],
            recv.at[me, pl.ds(g * G, G)],
            st_send.at[g, k],
            st_recv.at[g, k],
            device_id=at(k),
            device_id_type=MESH,
        )

    off_load.wait()
    later_ones = ones_where((L, L), lambda t, u: u > t)

    def step(g, carry):
        load_x(g).wait()
        xg = xbuf[pl.ds(g * G, G)].reshape(G * L, xbuf.shape[2])
        acc = jnp.dot(xg, wall[...], preferred_element_type=F32).astype(BF16).astype(F32)

        @pl.when(g == 0)
        def _():
            @pl.when(me == 0)
            def _():
                halo[...] = jnp.zeros_like(halo)

            @pl.when(me > 0)
            def _():
                halo_copy().wait_recv()
                halo[...] = halo_in[...].astype(F32)

        for q in range(G):
            p = g * G + q
            raw = acc[q * L : (q + 1) * L]
            pad[q, 8 : 8 + L, :] = raw[:, 0:C]
            for j in range(CONV - 1):
                r = 8 - (CONV - 1) + j
                pad[q, r : r + 1, :] = halo[j, pl.ds(p, 1), :]
            dt = softplus(raw[:, C : C + HEADS] + bias)
            ld = off[p] - speed * dt
            suffix = exact_dot(later_ones, ld)
            logs_out[pl.ds(p, 1), 0:HEADS] = suffix[0:1] + ld[0:1]
            w = dt * jnp.exp(suffix)
            hi = w.astype(BF16)
            lo = (w - hi.astype(F32)).astype(BF16)
            wide = jnp.dot(
                jnp.concatenate([hi, lo], axis=1), expand[...], preferred_element_type=F32
            )

            def mixed(c):
                s = slice(c, c + 128)
                t = pad[q, 8 - (CONV - 1) : 8 - (CONV - 1) + L, s] * taps[0:1, s]
                for j in range(1, CONV):
                    r = 8 - (CONV - 1) + j
                    t = t + pad[q, r : r + L, s] * taps[j : j + 1, s]
                return silu(t).astype(BF16)

            in_map = mixed(F)
            for c in range(0, F, 128):
                weighted = (mixed(c).astype(F32) * wide[:, c : c + 128]).astype(BF16)
                share = lax.dot_general(
                    weighted, in_map, (((0,), (0,)), ((), ())), preferred_element_type=F32
                ).astype(BF16)
                for hh in range(128 // P_SIZE):
                    h = c // P_SIZE + hh
                    for d in range(n):
                        b = hh * P_SIZE + d * R
                        sendbuf[d, p, h * R : (h + 1) * R, :] = share[b : b + R]
        for k in range(1, n):
            state_copy(g, k).start()
        return carry

    lax.fori_loop(0, steps, step, 0)

    def log_copy(k):
        return pltpu.make_async_remote_copy(
            logs_out, logs.at[me], log_send.at[k], log_recv.at[k], device_id=at(k), device_id_type=MESH
        )

    for k in range(1, n):
        log_copy(k).start()
    logs[me] = logs_out[...]
    recv[me] = sendbuf[me]

    RH = heads * R
    head_rows = ones_where((RH, HEADS), lambda l, i: i == lead + lax.div(l, R))
    head_cols = ones_where((HEADS, RH), lambda i, l: i == lead + lax.div(l, R))
    pick = ones_where(
        (F, RH), lambda c, l: c == lax.div(l, R) * P_SIZE + me * R + lax.rem(l, R), BF16
    )
    row_pick = ones_where((P_SIZE, RH), lambda c, l: c == me * R + lax.rem(l, R))
    gate_load.wait()
    gate = jnp.dot(edge[S], wg[...], preferred_element_type=F32).astype(BF16)
    gate_here = silu(jnp.dot(gate, pick, preferred_element_type=F32))
    gain_here = jnp.sum(exact_dot(gain_ref[...], row_pick) * head_cols, axis=0, keepdims=True)
    skip_here = exact_dot(skip_ref[...], head_cols)
    new_dt = softplus(new_step + bias)
    dt_here = exact_dot(new_dt, head_cols)
    keep_here = jnp.exp(-exact_dot(speed * new_dt, head_cols))

    @pl.when(me < n - 1)
    def _():
        pltpu.make_async_remote_copy(
            newest, newest, new_send.at[0], new_recv, device_id=at(1), device_id_type=MESH
        ).wait_recv()

    new_mixed = silu(newest[0] + new_raw * taps[CONV - 1 : CONV, :]).astype(BF16)
    new_input = jnp.dot(new_mixed[:, 0:F], pick, preferred_element_type=F32)
    new_in = new_mixed[:, F:C].astype(F32)
    new_out = new_mixed[:, C : C + STATE]
    both = jnp.sum(new_in * new_out.astype(F32), axis=1, keepdims=True)

    for k in range(1, n):
        log_copy(k).wait_recv()
    later = jnp.zeros(logs_out.shape, F32)
    factors = [None] * n
    for s in reversed(range(n)):
        factors[s] = exact_dot(head_rows, jnp.exp(later)[:, 0:HEADS], ((1,), (1,)))
        later = later + logs[s]

    where_row = lax.broadcasted_iota(jnp.int32, (SP, RH), 0)
    y = jnp.zeros((SP, RH), F32)
    for g in range(steps):
        for k in range(1, n):
            state_copy(g, k).wait_recv()
        for p in range(g * G, (g + 1) * G):
            tot = factors[0][:, p : p + 1] * recv[0, p].astype(F32)
            for s in range(1, n):
                tot = tot + factors[s][:, p : p + 1] * recv[s, p].astype(F32)
            kept = tot.astype(BF16)
            cache_ref[p] = kept
            part = lax.dot_general(
                new_out, kept, (((1,), (1,)), ((), ())), preferred_element_type=F32
            )
            y = jnp.where(where_row == p, part, y)
    readout = keep_here * y + dt_here * new_input * both + skip_here * new_input
    gated = readout * gate_here
    sq = jnp.broadcast_to(jnp.sum(gated * gated, axis=1, keepdims=True), sq_out.shape)
    sq_out[...] = sq

    def sq_copy(i):
        a, b = peers[i]
        return pltpu.make_async_remote_copy(
            sq_out, sq_in.at[i], sq_send.at[i], sq_recv.at[i], device_id=at(a, b), device_id_type=MESH
        )

    for i in range(len(peers)):
        sq_copy(i).start()
    for i in range(len(peers)):
        sq_copy(i).wait_recv()
        sq = sq + sq_in[i]
    scale = lax.rsqrt(sq[:, 0:1] / (HEADS * P_SIZE) + epsilon)
    read_ref[...] = (gated * scale * gain_here).astype(BF16)[0:S]

    for i in range(len(peers)):
        sq_copy(i).wait_send()
    for k in range(1, n):
        log_copy(k).wait_send()
        for g in range(steps):
            state_copy(g, k).wait_send()

    @pl.when(me < n - 1)
    def _():
        halo_copy().wait_send()

    @pl.when(me == n - 1)
    def _():
        for k in range(1, n):
            newest_copy(k).wait_send()


def fused(*args):
    x, wv, wk = args[0], args[2], args[4]
    S, L, D = x.shape
    n, m = lax.axis_size("sp"), lax.axis_size("tp")
    F = wv.shape[1]
    heads = F // P_SIZE
    R = P_SIZE // n
    G = next(g for g in (3, 2, 1) if S % g == 0)
    steps = S // G
    C, RH, SP = F + STATE, heads * R, 16
    dims = (n, m, S, L, heads, R, G)
    flat = list(args)
    for i in (10, 11, 12):
        flat[i] = args[i].reshape(1, HEADS)
    hbm, vmem = pl.BlockSpec(memory_space=pl.ANY), pl.BlockSpec(memory_space=pltpu.VMEM)
    specs = [hbm, vmem, hbm, hbm, hbm, hbm, hbm] + [vmem] * 7 + [hbm]
    dma = pltpu.SemaphoreType.DMA
    cache, read = pl.pallas_call(
        lambda *refs: mixer_kernel(dims, *refs),
        out_shape=(
            jax.ShapeDtypeStruct((S, RH, STATE), BF16),
            jax.ShapeDtypeStruct((S, RH), BF16),
        ),
        in_specs=specs,
        out_specs=(vmem, vmem),
        scratch_shapes=[
            pltpu.VMEM((S, L, D), BF16),
            pltpu.VMEM((S + 1, 16, D), BF16),
            pltpu.VMEM((D, C + STATE), BF16),
            pltpu.VMEM((D, STATE), BF16),
            pltpu.VMEM((D, HEADS), BF16),
            pltpu.VMEM((D, F), BF16),
            pltpu.VMEM((S, L, HEADS), F32),
            pltpu.VMEM((CONV, C + STATE), F32),
            pltpu.VMEM((G, 8 + L, C), F32),
            pltpu.VMEM((CONV - 1, SP, C), BF16),
            pltpu.VMEM((CONV - 1, SP, C), BF16),
            pltpu.VMEM((CONV - 1, SP, C), F32),
            pltpu.VMEM((1, SP, C + STATE), F32),
            pltpu.VMEM((SP, 128), F32),
            pltpu.VMEM((n, SP, 128), F32),
            pltpu.VMEM((n, S, RH, STATE), BF16),
            pltpu.VMEM((n, S, RH, STATE), BF16),
            pltpu.VMEM((SP, 128), F32),
            pltpu.VMEM((n * m - 1, SP, 128), F32),
            pltpu.VMEM((2 * HEADS, F), BF16),
            dma((7,)),
            dma((steps,)),
            dma((2,)),
            dma((n,)),
            dma,
            dma((steps, n)),
            dma((steps, n)),
            dma((n,)),
            dma((n,)),
            dma((n * m,)),
            dma((n * m,)),
        ],
        compiler_params=pltpu.CompilerParams(
            collective_id=0, has_side_effects=True, vmem_limit_bytes=56 * 1024 * 1024
        ),
    )(*flat)
    return cache.reshape(S, heads, R, STATE), read.reshape(S, heads, R)


def fits(n, m, shapes):
    (S, L), F = shapes
    heads, R = F // P_SIZE, P_SIZE // n
    return (
        n > 1
        and F % 128 == 0
        and R % 16 == 0
        and (heads * R) % 128 == 0
        and S <= 16
        and L % 16 == 0
        and L <= 128
        and (HEADS // GROUPS) % heads == 0
    )


def part(*args):
    shapes = (args[0].shape[:2], args[2].shape[1])
    if fits(lax.axis_size("sp"), lax.axis_size("tp"), shapes):
        return fused(*args)
    return shards(*args)


def solution(mesh):
    in_specs = (
        P("grp", "sp", None),
        P("grp", None),
        P(None, "tp"),
        P(None, "tp"),
        P(),
        P(),
        P(),
        P(),
        P(),
        P(),
        P(),
        P(),
        P(),
        P(),
        P("grp", "sp", None),
    )
    out_specs = (P("grp", "tp", "sp", None), P("grp", "tp", "sp"))
    return jax.shard_map(part, mesh=mesh, in_specs=in_specs, out_specs=out_specs, check_vma=False)
```

```python
import jax
import jax.numpy as jnp
from jax import lax
from jax.experimental import pallas as pl
from jax.experimental.pallas import tpu as pltpu
from jax.sharding import PartitionSpec as P

HEADS = 32
P_SIZE = 64
GROUPS = 2
STATE = 128
CONV = 4
SPAN = 64


epsilon = 1e-06


def shifted(block, axis, distance):
    devices = range(lax.axis_size(axis))
    route = [(i - distance, i) for i in devices if i - distance in devices]
    return lax.ppermute(block, axis, route)


def broadcast(value, axis, source):
    kept = jnp.where(lax.axis_index(axis) == source, value, 0).astype(value.dtype)
    return lax.psum(kept, axis)


def prefix(shard, axis, combine, identity):
    length, here = (lax.axis_size(axis), lax.axis_index(axis))
    everything = lax.all_gather(shard, axis)
    start = jnp.broadcast_to(jnp.asarray(identity, shard.dtype), shard.shape)

    def lap(k, before):
        at = length - 1 - k
        reached = at > here
        new = combine(before, everything[at])
        return jnp.where(reached, new, before)

    return lax.fori_loop(0, length, lap, start)


def shards(
    prompt_layer_input,
    next_token_input,
    value_projection,
    output_gate_matrix,
    key_projection,
    query_projection,
    step_projection,
    value_filter_taps,
    key_filter_taps,
    query_filter_taps,
    step_size_bias,
    head_decay_logarithm,
    direct_path_weight,
    gated_norm_gain,
    position_decay_offset,
):
    seq_count, local_len, width = prompt_layer_input.shape
    resident_heads = value_projection.shape[1] // P_SIZE
    feature_cols = resident_heads * P_SIZE
    shard_count = lax.axis_size("sp")
    rows_here = P_SIZE // shard_count
    shard_index = lax.axis_index("sp")
    leading_head = lax.axis_index("tp") * resident_heads
    group_index = leading_head // (HEADS // GROUPS)
    row_first = shard_index * rows_here
    in_cols = lax.dynamic_slice_in_dim(key_projection, group_index * STATE, STATE, 1)
    out_cols = lax.dynamic_slice_in_dim(query_projection, group_index * STATE, STATE, 1)
    weights_here = jnp.concatenate([value_projection, in_cols, out_cols], axis=1)
    step_cols = lax.dynamic_slice_in_dim(step_projection, leading_head, resident_heads, 1)
    kernel = jnp.concatenate(
        [
            lax.dynamic_slice_in_dim(value_filter_taps, leading_head * P_SIZE, feature_cols, 1),
            lax.dynamic_slice_in_dim(key_filter_taps, group_index * STATE, STATE, 1),
            lax.dynamic_slice_in_dim(query_filter_taps, group_index * STATE, STATE, 1),
        ],
        axis=1,
    ).astype(jnp.float32)
    head_decay_speed = jnp.exp(
        lax.dynamic_slice_in_dim(head_decay_logarithm, leading_head, resident_heads, 0)
    )
    bias_here = lax.dynamic_slice_in_dim(step_size_bias, leading_head, resident_heads, 0)
    skip_here = lax.dynamic_slice_in_dim(direct_path_weight, leading_head, resident_heads, 0)
    gain_here = lax.dynamic_slice(
        gated_norm_gain, (leading_head, row_first), (resident_heads, rows_here)
    )
    token_rows = prompt_layer_input.reshape(seq_count * local_len, width)
    projected = jnp.dot(token_rows, weights_here, preferred_element_type=jnp.float32).astype(
        jnp.bfloat16
    )
    projected = projected.reshape(seq_count, local_len, feature_cols + 2 * STATE)
    trailing = projected[:, local_len - (CONV - 1) :]
    before = shifted(trailing, "sp", 1)
    newest = broadcast(trailing, "sp", shard_count - 1)
    padded = jnp.concatenate([before, projected], axis=1)
    total = padded[:, 0:local_len].astype(jnp.float32) * kernel[0]
    for tap in range(1, CONV):
        total = total + padded[:, tap : tap + local_len].astype(jnp.float32) * kernel[tap]
    mixed = jax.nn.silu(total).astype(jnp.bfloat16)
    step_raw = jnp.dot(token_rows, step_cols, preferred_element_type=jnp.float32).astype(
        jnp.bfloat16
    )
    discrete_step = jax.nn.softplus(step_raw.astype(jnp.float32) + bias_here).reshape(
        seq_count, local_len, resident_heads
    )
    decay_spikes = lax.dynamic_slice_in_dim(position_decay_offset, leading_head, resident_heads, 2)
    logarithmic_decay = decay_spikes - head_decay_speed * discrete_step
    block_count = local_len // SPAN
    cumulative = jnp.cumsum(
        logarithmic_decay.reshape(seq_count, block_count, SPAN, resident_heads), axis=2
    )
    decay_weight = jnp.exp(cumulative[:, :, -1:] - cumulative) * discrete_step.reshape(
        seq_count, block_count, SPAN, resident_heads
    )
    head_input = mixed[:, :, :feature_cols].reshape(
        seq_count, block_count, SPAN, resident_heads, P_SIZE
    )
    weighted = (head_input.astype(jnp.float32) * decay_weight[..., None]).astype(jnp.bfloat16)
    in_map = mixed[:, :, feature_cols : feature_cols + STATE].reshape(
        seq_count, block_count, SPAN, STATE
    )
    block_state = jnp.einsum(
        "bcshp,bcsn->bchpn", weighted, in_map, preferred_element_type=jnp.float32
    )
    block_log = cumulative[:, :, -1]
    own_log = jnp.sum(block_log, axis=1)
    after_block = jnp.exp(own_log[:, None] - jnp.cumsum(block_log, axis=1))
    local_state = jnp.sum(after_block[..., None, None] * block_state, axis=1)
    later_log = prefix(own_log, "sp", jnp.add, jnp.zeros_like(own_log))
    scaled = jnp.exp(later_log)[:, :, None, None] * local_state
    own_rows = lax.psum_scatter(scaled, "sp", scatter_dimension=2, tiled=True)
    state_cache = own_rows.astype(jnp.bfloat16)
    new_raw = jnp.dot(next_token_input, weights_here, preferred_element_type=jnp.float32).astype(
        jnp.bfloat16
    )
    new_step = jnp.dot(next_token_input, step_cols, preferred_element_type=jnp.float32).astype(
        jnp.bfloat16
    )
    new_gate = jnp.dot(
        next_token_input, output_gate_matrix, preferred_element_type=jnp.float32
    ).astype(jnp.bfloat16)
    window = jnp.concatenate([newest, new_raw[:, None]], axis=1)
    new_mixed = jax.nn.silu(jnp.sum(window.astype(jnp.float32) * kernel[None], axis=1)).astype(
        jnp.bfloat16
    )
    new_input = lax.dynamic_slice_in_dim(
        new_mixed[:, :feature_cols].reshape(seq_count, resident_heads, P_SIZE),
        row_first,
        rows_here,
        2,
    ).astype(jnp.float32)
    new_in = new_mixed[:, feature_cols : feature_cols + STATE].astype(jnp.float32)
    new_out = new_mixed[:, feature_cols + STATE :].astype(jnp.float32)
    new_step_size = jax.nn.softplus(new_step.astype(jnp.float32) + bias_here)
    cache_values = lax.optimization_barrier(state_cache).astype(jnp.float32)
    new_state = (
        jnp.exp(-head_decay_speed * new_step_size)[:, :, None, None] * cache_values
        + (new_step_size[:, :, None] * new_input)[..., None] * new_in[:, None, None, :]
    )
    readout = (
        jnp.sum(new_state * new_out[:, None, None, :], axis=-1)
        + skip_here[None, :, None] * new_input
    )
    gate_rows = lax.dynamic_slice_in_dim(
        new_gate.reshape(seq_count, resident_heads, P_SIZE), row_first, rows_here, 2
    )
    gated = readout * jax.nn.silu(gate_rows.astype(jnp.float32))
    squares = lax.psum(jnp.sum(gated * gated, axis=(1, 2)), ("sp", "tp"))
    scale = lax.rsqrt(squares / (HEADS * P_SIZE) + epsilon)
    first_read = (gated * scale[:, None, None] * gain_here[None]).astype(jnp.bfloat16)
    return (state_cache, first_read)


F32, BF16 = jnp.float32, jnp.bfloat16
MESH = pl.DeviceIdType.MESH
EXACT = lax.Precision.HIGHEST


def exact_dot(a, b, dims=((1,), (0,))):
    return lax.dot_general(a, b, (dims, ((), ())), precision=EXACT, preferred_element_type=F32)


def softplus(v):
    return jnp.maximum(v, 0.0) + jnp.log1p(jnp.exp(-jnp.abs(v)))


def silu(v):
    return v / (1.0 + jnp.exp(-v))


def ones_where(shape, test, dtype=F32):
    rows = lax.broadcasted_iota(jnp.int32, shape, 0)
    cols = lax.broadcasted_iota(jnp.int32, shape, 1)
    return jnp.where(test(rows, cols), 1.0, 0.0).astype(dtype)


def mixer_kernel(
    dims,
    x_hbm,
    next_ref,
    wv_hbm,
    wg_hbm,
    wk_hbm,
    wq_hbm,
    ws_hbm,
    tv_ref,
    tk_ref,
    tq_ref,
    bias_ref,
    speed_ref,
    skip_ref,
    gain_ref,
    off_hbm,
    cache_ref,
    read_ref,
    xbuf,
    edge,
    wall,
    wq,
    ws,
    wg,
    off,
    taps,
    pad,
    halo_out,
    halo_in,
    halo,
    newest,
    logs_out,
    logs,
    sendbuf,
    recv,
    sq_out,
    sq_in,
    expand,
    load_sem,
    x_sem,
    halo_sem,
    new_send,
    new_recv,
    st_send,
    st_recv,
    log_send,
    log_recv,
    sq_send,
    sq_recv,
):
    n, m, S, L, heads, R, G = dims
    F = heads * P_SIZE
    C = F + STATE
    SP = sq_out.shape[0]
    steps = S // G
    me, tp = lax.axis_index("sp"), lax.axis_index("tp")
    lead = tp * heads
    group = lax.div(lead, HEADS // GROUPS)
    fcol = pl.multiple_of(tp * F, 128)
    gcol = pl.multiple_of(group * STATE, 128)

    def load(src, dst, k):
        c = pltpu.make_async_copy(src, dst, load_sem.at[k])
        c.start()
        return c

    def load_x(g):
        return pltpu.make_async_copy(
            x_hbm.at[pl.ds(g * G, G)], xbuf.at[pl.ds(g * G, G)], x_sem.at[g]
        )

    first = [
        load(x_hbm.at[:, pl.ds(L - 16, 16)], edge.at[pl.ds(0, S)], 0),
        load(wk_hbm.at[:, pl.ds(gcol, STATE)], wall.at[:, pl.ds(F, STATE)], 1),
        load(ws_hbm, ws, 2),
        load(wq_hbm.at[:, pl.ds(gcol, STATE)], wq, 3),
        load(wv_hbm, wall.at[:, pl.ds(0, F)], 4),
    ]
    for g in range(steps):
        load_x(g).start()
    off_load = load(off_hbm, off, 5)
    gate_load = load(wg_hbm, wg, 6)

    peers = [(a, b) for a in range(n) for b in range(m) if (a, b) != (0, 0)]

    def at(a, b=0):
        return {"sp": lax.rem(me + a, n), "tp": lax.rem(tp + b, m)}

    barrier = pltpu.get_barrier_semaphore()
    for a, b in peers:
        pl.semaphore_signal(barrier, inc=1, device_id=at(a, b), device_id_type=MESH)

    taps[:, 0:F] = tv_ref[:, pl.ds(fcol, F)].astype(F32)
    taps[:, F:C] = tk_ref[:, pl.ds(gcol, STATE)].astype(F32)
    taps[:, C : C + STATE] = tq_ref[:, pl.ds(gcol, STATE)].astype(F32)
    edge[S] = jnp.zeros(edge.shape[1:], BF16)
    edge[S, 0:S, :] = next_ref[...]
    halo_out[...] = jnp.zeros_like(halo_out)
    newest_zero = jnp.zeros(newest.shape[1:], F32)
    head_of = ones_where((HEADS, F), lambda i, c: i == lead + lax.div(c, P_SIZE), BF16)
    expand[0:HEADS, :] = head_of
    expand[HEADS : 2 * HEADS, :] = head_of
    bias = bias_ref[...]
    speed = jnp.exp(speed_ref[...])
    square = jnp.zeros((128, 128 - HEADS), F32)

    def columns(row):
        full = jnp.concatenate([jnp.broadcast_to(row, (128, HEADS)), square], axis=1)
        return full.T[0:HEADS]

    bias_t, speed_t = columns(bias), columns(speed)

    for c in first:
        c.wait()
    wall[:, C : C + STATE] = jnp.concatenate(
        [ws[...], jnp.zeros((STATE - HEADS, ws.shape[1]), BF16)], axis=0
    ).T
    rows = edge[...].reshape((S + 1) * 16, edge.shape[2])
    eproj = jnp.dot(rows, wall[...], preferred_element_type=F32).astype(BF16).astype(F32)
    eq = jnp.dot(rows, wq[...], preferred_element_type=F32).astype(BF16).astype(F32)
    e3 = eproj.reshape(S + 1, 16, C + STATE)
    q3 = eq.reshape(S + 1, 16, STATE)
    total = jnp.zeros((S, C + STATE), F32)
    for j in range(CONV - 1):
        row = 16 - (CONV - 1) + j
        tail = e3[0:S, row, 0:C]
        halo_out[j, 0:S, :] = tail.astype(BF16)
        total = total + jnp.concatenate([tail, q3[0:S, row, :]], axis=1) * taps[j : j + 1, :]
    new_raw = jnp.concatenate([e3[S, :, 0:C], q3[S]], axis=1)
    new_step = e3[S, :, C : C + HEADS]

    pl.semaphore_wait(barrier, len(peers))

    def halo_copy():
        return pltpu.make_async_remote_copy(
            halo_out, halo_in, halo_sem.at[0], halo_sem.at[1], device_id=at(1), device_id_type=MESH
        )

    @pl.when(me < n - 1)
    def _():
        halo_copy().start()

    def newest_copy(k):
        return pltpu.make_async_remote_copy(
            newest, newest, new_send.at[k], new_recv, device_id=at(k), device_id_type=MESH
        )

    @pl.when(me == n - 1)
    def _():
        newest[0] = newest_zero
        newest[0, 0:S, :] = total
        for k in range(1, n):
            newest_copy(k).start()

    def state_copy(g, k):
        to = lax.rem(me + k, n)
        return pltpu.make_async_remote_copy(
            sendbuf.at[to, pl.ds(g * G, G)],
            recv.at[me, pl.ds(g * G, G)],
            st_send.at[g, k],
            st_recv.at[g, k],
            device_id=at(k),
            device_id_type=MESH,
        )

    def log_copy(g, k):
        return pltpu.make_async_remote_copy(
            logs_out.at[pl.ds(g * G, G)],
            logs.at[me, pl.ds(g * G, G)],
            log_send.at[g, k],
            log_recv.at[g, k],
            device_id=at(k),
            device_id_type=MESH,
        )

    off_load.wait()
    later_ones = ones_where((L, L), lambda u, t: u > t)

    def step(g, carry):
        load_x(g).wait()
        xg = xbuf[pl.ds(g * G, G)].reshape(G * L, xbuf.shape[2])
        acc = jnp.dot(xg, wall[...], preferred_element_type=F32).astype(BF16).astype(F32)

        @pl.when(g == 0)
        def _():
            @pl.when(me == 0)
            def _():
                halo[...] = jnp.zeros_like(halo)

            @pl.when(me > 0)
            def _():
                halo_copy().wait_recv()
                halo[...] = halo_in[...].astype(F32)

        for q in range(G):
            p = g * G + q
            raw = acc[q * L : (q + 1) * L]
            pad[q, 8 : 8 + L, :] = raw[:, 0:C]
            for j in range(CONV - 1):
                r = 8 - (CONV - 1) + j
                pad[q, r : r + 1, :] = halo[j, pl.ds(p, 1), :]
            dt = softplus(raw[:, C : C + STATE].T[0:HEADS] + bias_t)
            ld = off[p] - speed_t * dt
            suffix = exact_dot(ld, later_ones)
            own = jnp.broadcast_to(suffix[:, 0:1] + ld[:, 0:1], (HEADS, 128))
            logs_out[p] = jnp.concatenate([own] * (128 // HEADS), axis=0).T[0:8]
            w = dt * jnp.exp(suffix)
            hi = w.astype(BF16)
            lo = (w - hi.astype(F32)).astype(BF16)
            wide = lax.dot_general(
                jnp.concatenate([hi, lo], axis=0),
                expand[...],
                (((0,), (0,)), ((), ())),
                preferred_element_type=F32,
            )

            def mixed(c):
                s = slice(c, c + 128)
                t = pad[q, 8 - (CONV - 1) : 8 - (CONV - 1) + L, s] * taps[0:1, s]
                for j in range(1, CONV):
                    r = 8 - (CONV - 1) + j
                    t = t + pad[q, r : r + L, s] * taps[j : j + 1, s]
                return silu(t).astype(BF16)

            in_map = mixed(F)
            for c in range(0, F, 128):
                weighted = (mixed(c).astype(F32) * wide[:, c : c + 128]).astype(BF16)
                share = lax.dot_general(
                    weighted, in_map, (((0,), (0,)), ((), ())), preferred_element_type=F32
                ).astype(BF16)
                for hh in range(128 // P_SIZE):
                    h = c // P_SIZE + hh
                    for d in range(n):
                        b = hh * P_SIZE + d * R
                        sendbuf[d, p, h * R : (h + 1) * R, :] = share[b : b + R]
        for k in range(1, n):
            log_copy(g, k).start()
        for k in range(1, n):
            state_copy(g, k).start()
        return carry

    lax.fori_loop(0, steps, step, 0)

    logs[me] = logs_out[...]
    recv[me] = sendbuf[me]

    RH = heads * R
    head_rows = ones_where((RH, HEADS), lambda l, i: i == lead + lax.div(l, R))
    head_cols = ones_where((HEADS, RH), lambda i, l: i == lead + lax.div(l, R))
    pick = ones_where(
        (F, RH), lambda c, l: c == lax.div(l, R) * P_SIZE + me * R + lax.rem(l, R), BF16
    )
    row_pick = ones_where((P_SIZE, RH), lambda c, l: c == me * R + lax.rem(l, R))
    gate_load.wait()
    gate = jnp.dot(edge[S], wg[...], preferred_element_type=F32).astype(BF16)
    gate_here = silu(jnp.dot(gate, pick, preferred_element_type=F32))
    gain_here = jnp.sum(exact_dot(gain_ref[...], row_pick) * head_cols, axis=0, keepdims=True)
    skip_here = exact_dot(skip_ref[...], head_cols)
    new_dt = softplus(new_step + bias)
    dt_here = exact_dot(new_dt, head_cols)
    keep_here = jnp.exp(-exact_dot(speed * new_dt, head_cols))

    @pl.when(me < n - 1)
    def _():
        pltpu.make_async_remote_copy(
            newest, newest, new_send.at[0], new_recv, device_id=at(1), device_id_type=MESH
        ).wait_recv()

    new_mixed = silu(newest[0] + new_raw * taps[CONV - 1 : CONV, :]).astype(BF16)
    new_input = jnp.dot(new_mixed[:, 0:F], pick, preferred_element_type=F32)
    new_in = new_mixed[:, F:C].astype(F32)
    new_out = new_mixed[:, C : C + STATE]
    both = jnp.sum(new_in * new_out.astype(F32), axis=1, keepdims=True)

    where_row = lax.broadcasted_iota(jnp.int32, (SP, RH), 0)
    y = jnp.zeros((SP, RH), F32)
    for g in range(steps):
        for k in range(1, n):
            log_copy(g, k).wait_recv()
            state_copy(g, k).wait_recv()
        for p in range(g * G, (g + 1) * G):
            later = jnp.zeros((1, HEADS), F32)
            tot = jnp.zeros((RH, STATE), F32)
            for s in reversed(range(n)):
                factor = jnp.sum(head_rows * jnp.exp(later), axis=1, keepdims=True)
                tot = tot + factor * recv[s, p].astype(F32)
                later = later + logs[s, p, 0:1, 0:HEADS]
            kept = tot.astype(BF16)
            cache_ref[p] = kept
            part = lax.dot_general(
                new_out, kept, (((1,), (1,)), ((), ())), preferred_element_type=F32
            )
            y = jnp.where(where_row == p, part, y)
    readout = keep_here * y + dt_here * new_input * both + skip_here * new_input
    gated = readout * gate_here
    sq = jnp.broadcast_to(jnp.sum(gated * gated, axis=1, keepdims=True), sq_out.shape)
    sq_out[...] = sq

    def sq_copy(i):
        a, b = peers[i]
        return pltpu.make_async_remote_copy(
            sq_out, sq_in.at[i], sq_send.at[i], sq_recv.at[i], device_id=at(a, b), device_id_type=MESH
        )

    for i in range(len(peers)):
        sq_copy(i).start()
    for i in range(len(peers)):
        sq_copy(i).wait_recv()
        sq = sq + sq_in[i]
    scale = lax.rsqrt(sq[:, 0:1] / (HEADS * P_SIZE) + epsilon)
    read_ref[...] = (gated * scale * gain_here).astype(BF16)[0:S]

    for i in range(len(peers)):
        sq_copy(i).wait_send()
    for k in range(1, n):
        for g in range(steps):
            log_copy(g, k).wait_send()
            state_copy(g, k).wait_send()

    @pl.when(me < n - 1)
    def _():
        halo_copy().wait_send()

    @pl.when(me == n - 1)
    def _():
        for k in range(1, n):
            newest_copy(k).wait_send()


def fused(*args):
    x, wv, wk = args[0], args[2], args[4]
    S, L, D = x.shape
    n, m = lax.axis_size("sp"), lax.axis_size("tp")
    F = wv.shape[1]
    heads = F // P_SIZE
    R = P_SIZE // n
    G = next(g for g in (2, 3, 1) if S % g == 0)
    steps = S // G
    C, RH, SP = F + STATE, heads * R, 16
    dims = (n, m, S, L, heads, R, G)
    flat = list(args)
    for i in (10, 11, 12):
        flat[i] = args[i].reshape(1, HEADS)
    flat[6] = args[6].T
    flat[14] = jnp.swapaxes(args[14], 1, 2)
    hbm, vmem = pl.BlockSpec(memory_space=pl.ANY), pl.BlockSpec(memory_space=pltpu.VMEM)
    specs = [hbm, vmem, hbm, hbm, hbm, hbm, hbm] + [vmem] * 7 + [hbm]
    dma = pltpu.SemaphoreType.DMA
    cache, read = pl.pallas_call(
        lambda *refs: mixer_kernel(dims, *refs),
        out_shape=(
            jax.ShapeDtypeStruct((S, RH, STATE), BF16),
            jax.ShapeDtypeStruct((S, RH), BF16),
        ),
        in_specs=specs,
        out_specs=(vmem, vmem),
        scratch_shapes=[
            pltpu.VMEM((S, L, D), BF16),
            pltpu.VMEM((S + 1, 16, D), BF16),
            pltpu.VMEM((D, C + STATE), BF16),
            pltpu.VMEM((D, STATE), BF16),
            pltpu.VMEM((HEADS, D), BF16),
            pltpu.VMEM((D, F), BF16),
            pltpu.VMEM((S, HEADS, L), F32),
            pltpu.VMEM((CONV, C + STATE), F32),
            pltpu.VMEM((G, 8 + L, C), F32),
            pltpu.VMEM((CONV - 1, SP, C), BF16),
            pltpu.VMEM((CONV - 1, SP, C), BF16),
            pltpu.VMEM((CONV - 1, SP, C), F32),
            pltpu.VMEM((1, SP, C + STATE), F32),
            pltpu.VMEM((S, 8, 128), F32),
            pltpu.VMEM((n, S, 8, 128), F32),
            pltpu.VMEM((n, S, RH, STATE), BF16),
            pltpu.VMEM((n, S, RH, STATE), BF16),
            pltpu.VMEM((SP, 128), F32),
            pltpu.VMEM((n * m - 1, SP, 128), F32),
            pltpu.VMEM((2 * HEADS, F), BF16),
            dma((7,)),
            dma((steps,)),
            dma((2,)),
            dma((n,)),
            dma,
            dma((steps, n)),
            dma((steps, n)),
            dma((steps, n)),
            dma((steps, n)),
            dma((n * m,)),
            dma((n * m,)),
        ],
        compiler_params=pltpu.CompilerParams(
            collective_id=0, has_side_effects=True, vmem_limit_bytes=56 * 1024 * 1024
        ),
    )(*flat)
    return cache.reshape(S, heads, R, STATE), read.reshape(S, heads, R)


def fits(n, m, shapes):
    (S, L), F = shapes
    heads, R = F // P_SIZE, P_SIZE // n
    return (
        n > 1
        and F % 128 == 0
        and R % 16 == 0
        and (heads * R) % 128 == 0
        and S <= 16
        and L % 16 == 0
        and L == 128
        and (HEADS // GROUPS) % heads == 0
    )


def part(*args):
    shapes = (args[0].shape[:2], args[2].shape[1])
    if fits(lax.axis_size("sp"), lax.axis_size("tp"), shapes):
        return fused(*args)
    return shards(*args)


def solution(mesh):
    in_specs = (
        P("grp", "sp", None),
        P("grp", None),
        P(None, "tp"),
        P(None, "tp"),
        P(),
        P(),
        P(),
        P(),
        P(),
        P(),
        P(),
        P(),
        P(),
        P(),
        P("grp", "sp", None),
    )
    out_specs = (P("grp", "tp", "sp", None), P("grp", "tp", "sp"))
    return jax.shard_map(part, mesh=mesh, in_specs=in_specs, out_specs=out_specs, check_vma=False)
```
